32 devices in a mesh: sp: 4 (over y, x), tp: 8 (over z, core).
Axes of the slice: x: 2, y: 2, z: 4, core: 2. Of those that a mesh axis runs over, the one named last changes fastest.
Arguments:
- tokens: bfloat16 [3, 2048, 4096], P(None, 'sp', 'tp'), may hold values from -6 to 6
- new_token: bfloat16 [3, 1, 4096], P(None, None, 'tp'), may hold values from -6 to 6
- query_weight: bfloat16 [4096, 4096], P(None, 'tp'), may hold values from -0.09375 to 0.09375
- key_weight: bfloat16 [4096, 4096], P(None, 'tp'), may hold values from -0.09375 to 0.09375
- value_weight: bfloat16 [4096, 4096], P(None, 'tp'), may hold values from -0.09375 to 0.09375
- log_decay: float32 [64], P('tp'), may hold values from -0.034 to 0
Outputs:
- state: bfloat16 [3, 64, 64, 64], P(None, 'tp', 'sp')
- read: bfloat16 [3, 4096], P(None, 'tp')
The draws below stay inside these ranges and needn't reach their ends.
All inputs are finite; a program needn't handle non-finite values.
Results may differ from the reference program's by a relative error of at most 0.012.
Values may be sent and summed in bfloat16 or wider, within the bound.
A program may use at most 64 MiB of HBM per device.

```python
import jax
import jax.numpy as jnp
from jax import lax

D = 4096
HEADS = 64
HD = 64
SEQS = 3
SPAN = 512
LEN = 2048
N_SP = 4


def draw_log_decay(key, part):
    choose_key = jax.random.fold_in(key, 11)
    fast_key = jax.random.fold_in(key, 12)
    slow_key = jax.random.fold_in(key, 13)
    chain_len = max(LEN, 64)
    fast_heads = jax.random.randint(choose_key, (HEADS,), 0, 2) == 1
    slow_rates = -jax.random.uniform(slow_key, (HEADS,), jnp.float32, 0.1, 2.0) / chain_len
    fast_rates = -1.0 / jax.random.uniform(fast_key, (HEADS,), jnp.float32, 30.0, 100.0)
    return jnp.where(fast_heads, fast_rates, slow_rates).astype(jnp.float32)


def shard_levels(own_key, dims, shards, low, top_value):
    def one(axis_at, parts):
        heights = jax.random.uniform(jax.random.fold_in(jax.random.fold_in(own_key, 6), axis_at), (parts,), jnp.float32, low / len(shards), top_value / len(shards))
        return jnp.repeat(jnp.exp(heights), dims[axis_at] // parts).reshape((-1,) + (1,) * (len(dims) - axis_at - 1))

    loudness = one(*shards[0])
    for cut in shards[1:]:
        loudness = loudness * one(*cut)
    return loudness


def bell_draw(rng, shape, spread, bound, pieces=(), kind=jnp.bfloat16):
    drawn = jax.random.normal(rng, shape, jnp.float32) * spread
    if len(pieces) > 0:
        drawn = shard_levels(rng, shape, pieces, -0.22, 0.18) * drawn
    return jnp.clip(drawn, min=-bound, max=bound).astype(kind)


def setup_inputs(seed: int = 0) -> dict:
    streams_of = jax.random.split(jax.random.key(seed), 7)
    return {
        "tokens": bell_draw(streams_of[0], (SEQS, LEN, D), 1.0, 6.0, ((1, 4), (2, 8))),
        "new_token": bell_draw(streams_of[1], (SEQS, 1, D), 1.0, 6.0, ((2, 8),)),
        "query_weight": bell_draw(streams_of[2], (D, HEADS * HD), D ** -0.5, 0.09375, ((1, 8),)),
        "key_weight": bell_draw(streams_of[3], (D, HEADS * HD), D ** -0.5, 0.09375, ((1, 8),)),
        "value_weight": bell_draw(streams_of[4], (D, HEADS * HD), D ** -0.5, 0.09375, ((1, 8),)),
        "log_decay": draw_log_decay(jax.random.fold_in(streams_of[6], 71), 0),
    }


def rotate(values, positions):
    half_dim = values.shape[-1] // 2
    inverse = 10000.0 ** (-jnp.arange(half_dim, dtype=jnp.float32) / half_dim)
    angles = positions.astype(jnp.float32)[:, None, None] * inverse[None, None, :]
    cosine = jnp.cos(angles)
    sine_part = jnp.sin(angles)
    first = values[..., :half_dim]
    second = values[..., half_dim:]
    return jnp.concatenate([first * cosine - second * sine_part, first * sine_part + second * cosine], axis=-1)

def group_norm(output):
    centered = output - lax.optimization_barrier(jnp.mean(output, axis=-1, keepdims=True))
    return centered * lax.rsqrt(lax.optimization_barrier(jnp.mean(centered * centered, axis=-1, keepdims=True)) + 1e-05)

def reference(tokens, new_token, query_weight, key_weight, value_weight, log_decay):
    key_scale = HD ** (-0.5)
    positions = jnp.arange(LEN, dtype=jnp.int32)
    to_end = (SPAN - 1 - positions % SPAN).astype(jnp.float32)
    block_ids = jnp.arange(N_SP, dtype=jnp.float32)
    new_position = jnp.full((1,), LEN, jnp.int32)
    query_heads = query_weight.reshape(D, HEADS, HD).transpose(1, 0, 2)
    key_heads = key_weight.reshape(D, HEADS, HD).transpose(1, 0, 2)
    value_heads = value_weight.reshape(D, HEADS, HD).transpose(1, 0, 2)

    def single_head(inputs):
        w_query, w_key, w_value, logarithm_rate = inputs
        projected = jnp.dot(tokens, w_key, preferred_element_type=jnp.float32)[:, :, None, :]
        key_rows = (rotate(projected, positions) * key_scale).astype(jnp.bfloat16)[:, :, 0, :]
        value_rows = jnp.dot(tokens, w_value, preferred_element_type=jnp.float32).astype(jnp.bfloat16)
        weighted = (key_rows.astype(jnp.float32) * jnp.exp(logarithm_rate * to_end)[None, :, None]).astype(jnp.bfloat16)
        weighted = weighted.astype(jnp.float32).reshape(SEQS, N_SP, SPAN, HD)
        value_blocks = value_rows.astype(jnp.float32).reshape(SEQS, N_SP, SPAN, HD)
        segment_states = jnp.einsum('sbtk,sbtv->sbkv', weighted, value_blocks, precision=lax.Precision.HIGHEST)
        carried_state = jnp.exp(logarithm_rate * SPAN * (N_SP - 1 - block_ids))
        closing_state = jnp.einsum('eyzt,y->ezt', segment_states, carried_state, precision=lax.Precision.HIGHEST)
        new_query = rotate(jnp.dot(new_token, w_query, preferred_element_type=jnp.float32)[:, :, None, :], new_position)
        new_query = new_query.astype(jnp.bfloat16)[:, 0, 0, :]
        fresh_key = rotate(jnp.dot(new_token, w_key, preferred_element_type=jnp.float32)[:, :, None, :], new_position)
        fresh_key = (fresh_key * key_scale).astype(jnp.bfloat16)[:, 0, 0, :]
        new_value = jnp.dot(new_token, w_value, preferred_element_type=jnp.float32).astype(jnp.bfloat16)[:, 0, :]
        query_entries = new_query.astype(jnp.float32)
        unscaled_read = jnp.exp(logarithm_rate) * jnp.einsum('bol,bo->bl', closing_state, query_entries, precision=lax.Precision.HIGHEST)
        unscaled_read = unscaled_read + lax.optimization_barrier(jnp.sum(query_entries * fresh_key.astype(jnp.float32), axis=-1, keepdims=True)) * new_value.astype(jnp.float32)
        return (closing_state.astype(jnp.bfloat16), group_norm(unscaled_read).astype(jnp.bfloat16))
    states, reads = lax.map(single_head, (query_heads, key_heads, value_heads, log_decay))
    return (states.transpose(1, 0, 2, 3), reads.transpose(1, 0, 2).reshape(SEQS, HEADS * HD))
```

```python
import functools

import jax
import jax.numpy as jnp
from jax import lax
from jax.experimental import pallas as pl
from jax.experimental.pallas import tpu as pltpu
from jax.sharding import PartitionSpec as P

HD = 64
LANES = 128
NEW_ROWS = 8
F32 = jnp.float32
BF16 = jnp.bfloat16


def lane_iota(shape):
    return lax.broadcasted_iota(jnp.int32, shape, len(shape) - 1)


def rotated(block, cosine, sine):
    half = HD // 2
    low = lane_iota(block.shape) % HD < half
    swapped = jnp.where(
        low, pltpu.roll(block, LANES - half, 1), pltpu.roll(block, half, 1)
    )
    return block * cosine + swapped * sine


def kernel(
    n_sp, n_tp,
    tokens, fresh, wq_hbm, wk_hbm, wv_hbm, inverse_ref, decay_ref,
    state_out, read_out,
    x, nx, wq, wk, wv, acc_k, acc_v, cos_ref, sin_ref, fade_ref, rows_ref,
    q_spread, own_term, stage, landed, totals,
    load_sem, weight_sem, rx, rn, fwd, share, nfwd, nshare, rs_tx, rs_rx,
):
    seqs, span, feat = tokens.shape
    inner = wk.shape[1]
    heads = inner // HD
    chips = n_tp // 2
    keep = HD // n_sp
    sp = lax.axis_index("sp")
    tp = lax.axis_index("tp")
    z, k = tp // 2, tp % 2
    MESH = pl.DeviceIdType.MESH

    def to_tp(index):
        return {"tp": index}

    partner = z * 2 + 1 - k
    own_loads = [
        pltpu.make_async_copy(tokens.at[s], x.at[tp, s], load_sem.at[s]) for s in range(seqs)
    ]
    new_load = pltpu.make_async_copy(fresh, nx.at[tp], load_sem.at[seqs])
    new_load.start()
    for copy in own_loads:
        copy.start()
    weight_loads = [
        pltpu.make_async_copy(a, b, weight_sem.at[i])
        for i, (a, b) in enumerate(((wk_hbm, wk), (wv_hbm, wv), (wq_hbm, wq)))
    ]
    for copy in weight_loads:
        copy.start()

    barrier = pltpu.get_barrier_semaphore()

    @pl.when(z > 0)
    def _():
        pl.semaphore_signal(barrier, inc=1, device_id=to_tp(tp - 2), device_id_type=MESH)

    @pl.when(z < chips - 1)
    def _():
        pl.semaphore_signal(barrier, inc=1, device_id=to_tp(tp + 2), device_id_type=MESH)

    pl.semaphore_signal(barrier, inc=1, device_id=to_tp(partner), device_id_type=MESH)
    for o in range(1, n_sp):
        pl.semaphore_signal(
            barrier, inc=1, device_id={"sp": lax.rem(sp + o, n_sp)}, device_id_type=MESH
        )
    pl.semaphore_wait(
        barrier, n_sp + (z > 0).astype(jnp.int32) + (z < chips - 1).astype(jnp.int32)
    )

    def x_copy(c, s, sem, target):
        p = 2 * c + k
        return pltpu.make_async_remote_copy(
            x.at[p, s], x.at[p, s], sem, rx.at[p, s], device_id=to_tp(target), device_id_type=MESH
        )

    def n_copy(c, sem, target):
        p = 2 * c + k
        return pltpu.make_async_remote_copy(
            nx.at[p], nx.at[p], sem, rn.at[p], device_id=to_tp(target), device_id_type=MESH
        )

    def x_arrived(p, s):
        pltpu.make_async_remote_copy(
            x.at[p, s], x.at[p, s], share.at[0, 0], rx.at[p, s],
            device_id=to_tp(partner), device_id_type=MESH,
        ).wait_recv()

    def n_arrived(p):
        pltpu.make_async_remote_copy(
            nx.at[p], nx.at[p], nshare.at[0], rn.at[p],
            device_id=to_tp(partner), device_id_type=MESH,
        ).wait_recv()

    new_load.wait()
    n_up = n_copy(z, nfwd.at[0, z], tp + 2)
    n_down = n_copy(z, nfwd.at[1, z], tp - 2)
    n_side = n_copy(z, nshare.at[z], partner)

    @pl.when(z < chips - 1)
    def _():
        n_up.start()

    @pl.when(z > 0)
    def _():
        n_down.start()

    n_side.start()
    for s in range(seqs):
        own_loads[s].wait()

        @pl.when(z < chips - 1)
        def _(s=s):
            x_copy(z, s, fwd.at[0, z, s], tp + 2).start()

        @pl.when(z > 0)
        def _(s=s):
            x_copy(z, s, fwd.at[1, z, s], tp - 2).start()

        x_copy(z, s, share.at[z, s], partner).start()

    row = lax.broadcasted_iota(jnp.int32, (span, LANES), 0)
    within = lane_iota((1, LANES)) % HD
    first_half = jnp.where(within < HD // 2, -1.0, 1.0).astype(F32)
    inverse = inverse_ref[...]
    angles = (sp * span + row).astype(F32) * inverse
    cos_ref[...] = jnp.cos(angles)
    sin_ref[...] = jnp.sin(angles) * first_half
    new_angles = jnp.full((NEW_ROWS, LANES), n_sp * span, F32) * inverse
    new_cos = jnp.cos(new_angles)
    new_sin = jnp.sin(new_angles) * first_half
    head_of = lane_iota((1, inner)) // HD
    rate = jnp.zeros((1, inner), F32)
    for h in range(heads):
        rate = jnp.where(head_of == h, decay_ref[h], rate)
    to_end = (span - 1 - lax.broadcasted_iota(jnp.int32, (span, 1), 0)).astype(F32)
    fade_ref[...] = jnp.exp(to_end * rate)
    rows_ref[0:1] = jnp.exp(rate * (span * (n_sp - 1 - sp)).astype(F32))
    rows_ref[1:2] = jnp.exp(rate)

    for copy in weight_loads:
        copy.wait()

    def add(p, s, fresh_total):
        block = x[p, s]
        where = pl.ds(pl.multiple_of(p * feat, feat), feat)
        part_k = jnp.dot(block, wk[where, :], preferred_element_type=F32)
        part_v = jnp.dot(block, wv[where, :], preferred_element_type=F32)
        if fresh_total:
            acc_k[s] = part_k
            acc_v[s] = part_v
        else:
            acc_k[s] += part_k
            acc_v[s] += part_v

    @pl.loop(0, seqs)
    def _(s):
        add(tp, s, True)
        x_arrived(partner, s)
        add(partner, s, False)

    n_arrived(partner)

    def project_new():
        def piece(p, totals):
            where = pl.ds(pl.multiple_of(p * feat, feat), feat)
            block = nx[p]
            return tuple(
                t + jnp.dot(block, w[where, :], preferred_element_type=F32)
                for t, w in zip(totals, (wk, wv, wq))
            )

        zero = jnp.zeros((NEW_ROWS, inner), F32)
        new_k, new_v, new_q = lax.fori_loop(0, n_tp, piece, (zero, zero, zero))
        keys, queries = [], []
        for j in range(inner // LANES):
            at = slice(j * LANES, (j + 1) * LANES)
            keys.append((rotated(new_k[:, at], new_cos, new_sin) * HD**-0.5).astype(BF16))
            queries.append(rotated(new_q[:, at], new_cos, new_sin).astype(BF16))
        key = jnp.concatenate(keys, axis=1).astype(F32)
        query = jnp.concatenate(queries, axis=1).astype(F32)
        value = new_v.astype(BF16).astype(F32)
        same = (
            lax.broadcasted_iota(jnp.int32, (inner, inner), 0) // HD
            == lax.broadcasted_iota(jnp.int32, (inner, inner), 1) // HD
        )
        product = query * key
        for h in range(heads):
            at = slice(h * HD, (h + 1) * HD)
            own_term[:, at] = jnp.sum(product[:, at], axis=-1, keepdims=True) * value[:, at]
        pick = lax.broadcasted_iota(jnp.int32, (HD, inner), 0) == lane_iota((HD, inner)) % HD
        for s in range(seqs):
            spread = jnp.where(pick, query[s : s + 1], 0.0).astype(BF16)
            q_spread[s] = jnp.dot(
                spread, jnp.where(same, 1.0, 0.0).astype(BF16), preferred_element_type=F32
            )

    def rs_copy(s, o):
        peer = lax.rem(sp + o, n_sp)
        return pltpu.make_async_remote_copy(
            stage.at[s, peer], landed.at[s, sp], rs_tx.at[s, peer], rs_rx.at[s, sp],
            device_id={"sp": peer}, device_id_type=MESH,
        )

    def finish(s):
        cosine, sine = cos_ref[...], sin_ref[...]
        lane = lane_iota((HD, LANES))
        for j in range(inner // LANES):
            at = slice(j * LANES, (j + 1) * LANES)
            key = (rotated(acc_k[s, :, at], cosine, sine) * HD**-0.5).astype(BF16)
            weighted = (key.astype(F32) * fade_ref[:, at]).astype(BF16)
            value = acc_v[s, :, at].astype(BF16)
            both = lax.dot_general(
                weighted, value, (((0,), (0,)), ((), ())), preferred_element_type=F32
            )
            state = jnp.where(lane < HD, both[:HD], both[HD:]) * rows_ref[0:1, at]
            part = jnp.sum(state * q_spread[s, :, at], axis=0, keepdims=True)
            for o in range(n_sp):
                stage[s, o, 0:keep, at] = state[o * keep : (o + 1) * keep]
                stage[s, o, keep : keep + 1, at] = part
        for o in range(1, n_sp):
            rs_copy(s, o).start()
        landed_own = stage[s, sp]
        totals[s] = landed_own

    far = jnp.maximum(z, chips - 1 - z)

    def decode(i):
        d = i // (2 * seqs) + 1
        s = (i // 2) % seqs
        step = 2 * (i % 2) - 1
        c = z + step * d
        return d, s, step, c, (c >= 0) & (c < chips)

    def onward(step):
        nxt = z - step
        return nxt, (nxt >= 0) & (nxt < chips), (step + 1) // 2

    @pl.loop(0, 2 * seqs * (chips - 1))
    def _(i):
        d, s, step, c, valid = decode(i)
        nxt, pass_on, way = onward(step)

        @pl.when(valid)
        def _():
            @pl.when(s == 0)
            def _():
                n_arrived(2 * c + k)

                @pl.when(pass_on)
                def _():
                    n_copy(c, nfwd.at[way, c], 2 * nxt + k).start()

                n_copy(c, nshare.at[c], partner).start()

            x_arrived(2 * c + k, s)

            @pl.when(pass_on)
            def _():
                x_copy(c, s, fwd.at[way, c, s], 2 * nxt + k).start()

            x_copy(c, s, share.at[c, s], partner).start()
            add(2 * c + k, s, False)

            @pl.when(s == 0)
            def _():
                n_arrived(2 * c + 1 - k)

            x_arrived(2 * c + 1 - k, s)
            add(2 * c + 1 - k, s, False)

        last = (d == far) & (step == 1)

        @pl.when(last & (s == 0))
        def _():
            project_new()

        @pl.when(last)
        def _():
            finish(s)

    raws = []
    for s in range(seqs):
        for o in range(1, n_sp):
            src = lax.rem(sp + o, n_sp)
            pltpu.make_async_remote_copy(
                stage.at[s, src], landed.at[s, src], rs_tx.at[s, src], rs_rx.at[s, src],
                device_id={"sp": src}, device_id_type=MESH,
            ).wait_recv()
        total = None
        for j in range(n_sp):
            term = jnp.where(sp == j, totals[s], landed[s, j])
            total = term if total is None else total + term
        kept = total[0:keep].astype(BF16)
        for h in range(heads):
            state_out[s, h] = kept[:, h * HD : (h + 1) * HD]
        raws.append(total[keep : keep + 1] * rows_ref[1:2] + own_term[s : s + 1])
    raw = jnp.concatenate(raws, axis=0)
    for h in range(heads):
        at = slice(h * HD, (h + 1) * HD)
        head = raw[:, at]
        centered = head - jnp.mean(head, axis=-1, keepdims=True)
        spread = jnp.mean(centered * centered, axis=-1, keepdims=True)
        read_out[:, at] = (centered * lax.rsqrt(spread + 1e-05)).astype(BF16)

    @pl.when(z < chips - 1)
    def _():
        n_up.wait_send()

    @pl.when(z > 0)
    def _():
        n_down.wait_send()

    n_side.wait_send()
    for s in range(seqs):
        @pl.when(z < chips - 1)
        def _(s=s):
            x_copy(z, s, fwd.at[0, z, s], tp + 2).wait_send()

        @pl.when(z > 0)
        def _(s=s):
            x_copy(z, s, fwd.at[1, z, s], tp - 2).wait_send()

        x_copy(z, s, share.at[z, s], partner).wait_send()
        for o in range(1, n_sp):
            rs_copy(s, o).wait_send()

    @pl.loop(0, 2 * seqs * (chips - 1))
    def _(i):
        d, s, step, c, valid = decode(i)
        nxt, pass_on, way = onward(step)

        @pl.when(valid)
        def _():
            @pl.when(s == 0)
            def _():
                @pl.when(pass_on)
                def _():
                    n_copy(c, nfwd.at[way, c], 2 * nxt + k).wait_send()

                n_copy(c, nshare.at[c], partner).wait_send()

            @pl.when(pass_on)
            def _():
                x_copy(c, s, fwd.at[way, c, s], 2 * nxt + k).wait_send()

            x_copy(c, s, share.at[c, s], partner).wait_send()


def solution(mesh):
    n_sp, n_tp = mesh.shape["sp"], mesh.shape["tp"]

    def body(tokens, new_token, query_weight, key_weight, value_weight, log_decay):
        seqs, span, feat = tokens.shape
        width, inner = key_weight.shape
        heads = inner // HD
        keep = HD // n_sp
        rows = -(-(keep + 1) // 8) * 8
        chips = n_tp // 2
        half = HD // 2
        inverse = 10000.0 ** (-jnp.arange(half, dtype=F32) / half)
        inverse = jnp.tile(inverse, LANES // half)[None]
        fresh = jnp.pad(new_token[:, 0], ((0, NEW_ROWS - seqs), (0, 0)))
        anywhere = pl.BlockSpec(memory_space=pl.ANY)
        vmem = pl.BlockSpec(memory_space=pltpu.VMEM)
        dma = pltpu.SemaphoreType.DMA
        return pl.pallas_call(
            functools.partial(kernel, n_sp, n_tp),
            out_shape=(
                jax.ShapeDtypeStruct((seqs, heads, keep, HD), BF16),
                jax.ShapeDtypeStruct((seqs, inner), BF16),
            ),
            in_specs=[anywhere] * 5 + [vmem, pl.BlockSpec(memory_space=pltpu.SMEM)],
            out_specs=(vmem, vmem),
            scratch_shapes=[
                pltpu.VMEM((n_tp, seqs, span, feat), BF16),
                pltpu.VMEM((n_tp, NEW_ROWS, feat), BF16),
                pltpu.VMEM((width, inner), BF16),
                pltpu.VMEM((width, inner), BF16),
                pltpu.VMEM((width, inner), BF16),
                pltpu.VMEM((seqs, span, inner), F32),
                pltpu.VMEM((seqs, span, inner), F32),
                pltpu.VMEM((span, LANES), F32),
                pltpu.VMEM((span, LANES), F32),
                pltpu.VMEM((span, inner), F32),
                pltpu.VMEM((8, inner), F32),
                pltpu.VMEM((seqs, HD, inner), F32),
                pltpu.VMEM((NEW_ROWS, inner), F32),
                pltpu.VMEM((seqs, n_sp, rows, inner), F32),
                pltpu.VMEM((seqs, n_sp, rows, inner), F32),
                pltpu.VMEM((seqs, rows, inner), F32),
                dma((seqs + 1,)),
                dma((3,)),
                dma((n_tp, seqs)),
                dma((n_tp,)),
                dma((2, chips, seqs)),
                dma((chips, seqs)),
                dma((2, chips)),
                dma((chips,)),
                dma((seqs, n_sp)),
                dma((seqs, n_sp)),
            ],
            compiler_params=pltpu.CompilerParams(
                collective_id=0, has_side_effects=True, vmem_limit_bytes=60 * 1024 * 1024
            ),
            name="retention",
        )(tokens, fresh, query_weight, key_weight, value_weight, inverse, log_decay)

    return jax.shard_map(
        body,
        mesh=mesh,
        in_specs=(
            P(None, "sp", "tp"),
            P(None, None, "tp"),
            P(None, "tp"),
            P(None, "tp"),
            P(None, "tp"),
            P("tp"),
        ),
        out_specs=(P(None, "tp", "sp", None), P(None, "tp")),
        check_vma=False,
    )
```

```python
import functools

import jax
import jax.numpy as jnp
import numpy as np
from jax import lax
from jax.experimental import pallas as pl
from jax.experimental.pallas import tpu as pltpu
from jax.sharding import PartitionSpec as P

HD = 64
LANES = 128
NEW_ROWS = 8
F32 = jnp.float32
BF16 = jnp.bfloat16


def lane_iota(shape):
    return lax.broadcasted_iota(jnp.int32, shape, len(shape) - 1)


def rotated(block, cosine, sine):
    half = HD // 2
    low = lane_iota(block.shape) % HD < half
    swapped = jnp.where(
        low, pltpu.roll(block, LANES - half, 1), pltpu.roll(block, half, 1)
    )
    return block * cosine + swapped * sine


def kernel(
    n_sp, n_tp, parts,
    tokens, fresh, wq_hbm, wk_hbm, wv_hbm, inverse_ref, decay_ref,
    state_out, read_out,
    x, nx, wq, wk, wv, acc_k, acc_v, cos_ref, sin_ref, fade_ref, rows_ref,
    q_spread, own_term, sums, stage, landed, totals,
    load_sem, weight_sem, rx, rn, fwd, share, nfwd, nshare, rs_tx, rs_rx,
):
    seqs, span, feat = tokens.shape
    inner = wk.shape[1]
    heads = inner // HD
    chips = n_tp // 2
    pieces = seqs * parts
    size = span // parts
    keep = HD // n_sp
    sp = lax.axis_index("sp")
    tp = lax.axis_index("tp")
    z, k = tp // 2, tp % 2
    MESH = pl.DeviceIdType.MESH

    def to_tp(index):
        return {"tp": index}

    partner = z * 2 + 1 - k
    own_loads = [
        pltpu.make_async_copy(
            tokens.at[s // parts, pl.ds(s % parts * size, size)], x.at[tp, s], load_sem.at[s]
        )
        for s in range(pieces)
    ]
    new_load = pltpu.make_async_copy(fresh, nx.at[tp], load_sem.at[pieces])
    new_load.start()
    for copy in own_loads:
        copy.start()
    weight_loads = [
        pltpu.make_async_copy(a, b, weight_sem.at[i])
        for i, (a, b) in enumerate(((wk_hbm, wk), (wv_hbm, wv), (wq_hbm, wq)))
    ]

    barrier = pltpu.get_barrier_semaphore()

    @pl.when(z > 0)
    def _():
        pl.semaphore_signal(barrier, inc=1, device_id=to_tp(tp - 2), device_id_type=MESH)

    @pl.when(z < chips - 1)
    def _():
        pl.semaphore_signal(barrier, inc=1, device_id=to_tp(tp + 2), device_id_type=MESH)

    pl.semaphore_signal(barrier, inc=1, device_id=to_tp(partner), device_id_type=MESH)
    for o in range(1, n_sp):
        pl.semaphore_signal(
            barrier, inc=1, device_id={"sp": lax.rem(sp + o, n_sp)}, device_id_type=MESH
        )
    pl.semaphore_wait(
        barrier, n_sp + (z > 0).astype(jnp.int32) + (z < chips - 1).astype(jnp.int32)
    )

    def x_copy(c, s, sem, target):
        p = 2 * c + k
        return pltpu.make_async_remote_copy(
            x.at[p, s], x.at[p, s], sem, rx.at[p, s], device_id=to_tp(target), device_id_type=MESH
        )

    def n_copy(c, sem, target):
        p = 2 * c + k
        return pltpu.make_async_remote_copy(
            nx.at[p], nx.at[p], sem, rn.at[p], device_id=to_tp(target), device_id_type=MESH
        )

    def x_arrived(p, s):
        pltpu.make_async_remote_copy(
            x.at[p, s], x.at[p, s], share.at[0, 0], rx.at[p, s],
            device_id=to_tp(partner), device_id_type=MESH,
        ).wait_recv()

    def n_arrived(p):
        pltpu.make_async_remote_copy(
            nx.at[p], nx.at[p], nshare.at[0], rn.at[p],
            device_id=to_tp(partner), device_id_type=MESH,
        ).wait_recv()

    new_load.wait()
    n_up = n_copy(z, nfwd.at[0, z], tp + 2)
    n_down = n_copy(z, nfwd.at[1, z], tp - 2)
    n_side = n_copy(z, nshare.at[z], partner)

    @pl.when(z < chips - 1)
    def _():
        n_up.start()

    @pl.when(z > 0)
    def _():
        n_down.start()

    n_side.start()
    for s in range(pieces):
        own_loads[s].wait()

        @pl.when(z < chips - 1)
        def _(s=s):
            x_copy(z, s, fwd.at[0, z, s], tp + 2).start()

        @pl.when(z > 0)
        def _(s=s):
            x_copy(z, s, fwd.at[1, z, s], tp - 2).start()

        x_copy(z, s, share.at[z, s], partner).start()

    for copy in weight_loads:
        copy.start()

    row = lax.broadcasted_iota(jnp.int32, (span, LANES), 0)
    within = lane_iota((1, LANES)) % HD
    first_half = jnp.where(within < HD // 2, -1.0, 1.0).astype(F32)
    inverse = inverse_ref[...]
    angles = (sp * span + row).astype(F32) * inverse
    cos_ref[...] = jnp.cos(angles)
    sin_ref[...] = jnp.sin(angles) * first_half
    new_angles = jnp.full((NEW_ROWS, LANES), n_sp * span, F32) * inverse
    new_cos = jnp.cos(new_angles)
    new_sin = jnp.sin(new_angles) * first_half
    head_of = lane_iota((1, inner)) // HD
    rate = jnp.zeros((1, inner), F32)
    for h in range(heads):
        rate = jnp.where(head_of == h, decay_ref[h], rate)
    to_end = (span - 1 - lax.broadcasted_iota(jnp.int32, (span, 1), 0)).astype(F32)
    fade_ref[...] = jnp.exp(to_end * rate)
    rows_ref[0:1] = jnp.exp(rate * (span * (n_sp - 1 - sp)).astype(F32))
    rows_ref[1:2] = jnp.exp(rate)

    for copy in weight_loads:
        copy.wait()

    def add(p, s, fresh_total):
        block = x[p, s]
        where = pl.ds(pl.multiple_of(p * feat, feat), feat)
        part_k = jnp.dot(block, wk[where, :], preferred_element_type=F32)
        part_v = jnp.dot(block, wv[where, :], preferred_element_type=F32)
        if fresh_total:
            acc_k[s] = part_k
            acc_v[s] = part_v
        else:
            acc_k[s] += part_k
            acc_v[s] += part_v

    @pl.loop(0, pieces)
    def _(s):
        add(tp, s, True)
        x_arrived(partner, s)
        add(partner, s, False)

    n_arrived(partner)

    def project_new():
        def piece(p, totals):
            where = pl.ds(pl.multiple_of(p * feat, feat), feat)
            block = jnp.concatenate(
                [nx[p].astype(F32), jnp.zeros((NEW_ROWS - seqs, feat), F32)], axis=0
            ).astype(BF16)
            return tuple(
                t + jnp.dot(block, w[where, :], preferred_element_type=F32)
                for t, w in zip(totals, (wk, wv, wq))
            )

        zero = jnp.zeros((NEW_ROWS, inner), F32)
        new_k, new_v, new_q = lax.fori_loop(0, n_tp, piece, (zero, zero, zero))
        keys, queries = [], []
        for j in range(inner // LANES):
            at = slice(j * LANES, (j + 1) * LANES)
            keys.append((rotated(new_k[:, at], new_cos, new_sin) * HD**-0.5).astype(BF16))
            queries.append(rotated(new_q[:, at], new_cos, new_sin).astype(BF16))
        key = jnp.concatenate(keys, axis=1).astype(F32)
        query = jnp.concatenate(queries, axis=1).astype(F32)
        value = new_v.astype(BF16).astype(F32)
        same = (
            lax.broadcasted_iota(jnp.int32, (inner, inner), 0) // HD
            == lax.broadcasted_iota(jnp.int32, (inner, inner), 1) // HD
        )
        product = query * key
        for h in range(heads):
            at = slice(h * HD, (h + 1) * HD)
            own_term[:, at] = jnp.sum(product[:, at], axis=-1, keepdims=True) * value[:, at]
        pick = lax.broadcasted_iota(jnp.int32, (HD, inner), 0) == lane_iota((HD, inner)) % HD
        for s in range(seqs):
            spread = jnp.where(pick, query[s : s + 1], 0.0).astype(BF16)
            q_spread[s] = jnp.dot(
                spread, jnp.where(same, 1.0, 0.0).astype(BF16), preferred_element_type=F32
            )

    def rs_copy(s, o):
        peer = lax.rem(sp + o, n_sp)
        return pltpu.make_async_remote_copy(
            stage.at[s, peer], landed.at[s, sp], rs_tx.at[s, peer], rs_rx.at[s, sp],
            device_id={"sp": peer}, device_id_type=MESH,
        )

    def finish(i):
        s, part = i // parts, i % parts
        where = pl.ds(pl.multiple_of(part * size, size), size)
        cosine, sine = cos_ref[where, :], sin_ref[where, :]
        lane = lane_iota((HD, LANES))
        for j in range(inner // LANES):
            at = slice(j * LANES, (j + 1) * LANES)
            key = (rotated(acc_k[i, :, at], cosine, sine) * HD**-0.5).astype(BF16)
            weighted = (key.astype(F32) * fade_ref[where, at]).astype(BF16)
            value = acc_v[i, :, at].astype(BF16)
            both = lax.dot_general(
                weighted, value, (((0,), (0,)), ((), ())), preferred_element_type=F32
            )
            state = jnp.where(lane < HD, both[:HD], both[HD:])
            sums[:, at] = jnp.where(part == 0, state, sums[:, at] + state)

        @pl.when(part == parts - 1)
        def _():
            scaled = sums[...] * rows_ref[0:1]
            read = jnp.sum(scaled * q_spread[s], axis=0, keepdims=True)
            for o in range(n_sp):
                stage[s, o, 0:keep] = scaled[o * keep : (o + 1) * keep]
                stage[s, o, keep : keep + 1] = read
            for o in range(1, n_sp):
                rs_copy(s, o).start()
            totals[s] = stage[s, sp]

    far = jnp.maximum(z, chips - 1 - z)

    def decode(i):
        d = i // (2 * pieces) + 1
        s = (i // 2) % pieces
        step = 2 * (i % 2) - 1
        c = z + step * d
        return d, s, step, c, (c >= 0) & (c < chips)

    def onward(step):
        nxt = z - step
        return nxt, (nxt >= 0) & (nxt < chips), (step + 1) // 2

    @pl.loop(0, 2 * pieces * (chips - 1))
    def _(i):
        d, s, step, c, valid = decode(i)
        nxt, pass_on, way = onward(step)

        @pl.when(valid)
        def _():
            @pl.when(s == 0)
            def _():
                n_arrived(2 * c + k)

                @pl.when(pass_on)
                def _():
                    n_copy(c, nfwd.at[way, c], 2 * nxt + k).start()

                n_copy(c, nshare.at[c], partner).start()

            x_arrived(2 * c + k, s)

            @pl.when(pass_on)
            def _():
                x_copy(c, s, fwd.at[way, c, s], 2 * nxt + k).start()

            x_copy(c, s, share.at[c, s], partner).start()
            add(2 * c + k, s, False)

            @pl.when(s == 0)
            def _():
                n_arrived(2 * c + 1 - k)

            x_arrived(2 * c + 1 - k, s)
            add(2 * c + 1 - k, s, False)

        last = (d == far) & (step == 1)

        @pl.when(last & (s == 0))
        def _():
            project_new()

        @pl.when(last)
        def _():
            finish(s)

    raws = []
    for s in range(seqs):
        for o in range(1, n_sp):
            src = lax.rem(sp + o, n_sp)
            pltpu.make_async_remote_copy(
                stage.at[s, src], landed.at[s, src], rs_tx.at[s, src], rs_rx.at[s, src],
                device_id={"sp": src}, device_id_type=MESH,
            ).wait_recv()
        total = None
        for j in range(n_sp):
            term = jnp.where(sp == j, totals[s], landed[s, j])
            total = term if total is None else total + term
        kept = total[0:keep].astype(BF16)
        for h in range(heads):
            state_out[s, h] = kept[:, h * HD : (h + 1) * HD]
        raws.append(total[keep : keep + 1] * rows_ref[1:2] + own_term[s : s + 1])
    raw = jnp.concatenate(raws, axis=0)
    for h in range(heads):
        at = slice(h * HD, (h + 1) * HD)
        head = raw[:, at]
        centered = head - jnp.mean(head, axis=-1, keepdims=True)
        spread = jnp.mean(centered * centered, axis=-1, keepdims=True)
        read_out[:, at] = (centered * lax.rsqrt(spread + 1e-05)).astype(BF16)

    @pl.when(z < chips - 1)
    def _():
        n_up.wait_send()

    @pl.when(z > 0)
    def _():
        n_down.wait_send()

    n_side.wait_send()
    for s in range(seqs):
        for o in range(1, n_sp):
            rs_copy(s, o).wait_send()
    for s in range(pieces):
        @pl.when(z < chips - 1)
        def _(s=s):
            x_copy(z, s, fwd.at[0, z, s], tp + 2).wait_send()

        @pl.when(z > 0)
        def _(s=s):
            x_copy(z, s, fwd.at[1, z, s], tp - 2).wait_send()

        x_copy(z, s, share.at[z, s], partner).wait_send()

    @pl.loop(0, 2 * pieces * (chips - 1))
    def _(i):
        d, s, step, c, valid = decode(i)
        nxt, pass_on, way = onward(step)

        @pl.when(valid)
        def _():
            @pl.when(s == 0)
            def _():
                @pl.when(pass_on)
                def _():
                    n_copy(c, nfwd.at[way, c], 2 * nxt + k).wait_send()

                n_copy(c, nshare.at[c], partner).wait_send()

            @pl.when(pass_on)
            def _():
                x_copy(c, s, fwd.at[way, c, s], 2 * nxt + k).wait_send()

            x_copy(c, s, share.at[c, s], partner).wait_send()


def solution(mesh):
    n_sp, n_tp = mesh.shape["sp"], mesh.shape["tp"]

    def body(tokens, new_token, query_weight, key_weight, value_weight, log_decay):
        seqs, span, feat = tokens.shape
        width, inner = key_weight.shape
        heads = inner // HD
        keep = HD // n_sp
        rows = -(-(keep + 1) // 8) * 8
        chips = n_tp // 2
        half = HD // 2
        parts = max(1, 8 // chips)
        pieces = seqs * parts
        inverse = np.float32(10000.0) ** (-np.arange(half, dtype=np.float32) / half)
        inverse = jnp.asarray(np.tile(inverse.astype(np.float32), LANES // half)[None])
        anywhere = pl.BlockSpec(memory_space=pl.ANY)
        vmem = pl.BlockSpec(memory_space=pltpu.VMEM)
        dma = pltpu.SemaphoreType.DMA
        return pl.pallas_call(
            functools.partial(kernel, n_sp, n_tp, parts),
            out_shape=(
                jax.ShapeDtypeStruct((seqs, heads, keep, HD), BF16),
                jax.ShapeDtypeStruct((seqs, inner), BF16),
            ),
            in_specs=[anywhere] * 5 + [vmem, pl.BlockSpec(memory_space=pltpu.SMEM)],
            out_specs=(vmem, vmem),
            scratch_shapes=[
                pltpu.VMEM((n_tp, pieces, span // parts, feat), BF16),
                pltpu.VMEM((n_tp, seqs, feat), BF16),
                pltpu.VMEM((width, inner), BF16),
                pltpu.VMEM((width, inner), BF16),
                pltpu.VMEM((width, inner), BF16),
                pltpu.VMEM((pieces, span // parts, inner), F32),
                pltpu.VMEM((pieces, span // parts, inner), F32),
                pltpu.VMEM((span, LANES), F32),
                pltpu.VMEM((span, LANES), F32),
                pltpu.VMEM((span, inner), F32),
                pltpu.VMEM((8, inner), F32),
                pltpu.VMEM((seqs, HD, inner), F32),
                pltpu.VMEM((NEW_ROWS, inner), F32),
                pltpu.VMEM((HD, inner), F32),
                pltpu.VMEM((seqs, n_sp, rows, inner), F32),
                pltpu.VMEM((seqs, n_sp, rows, inner), F32),
                pltpu.VMEM((seqs, rows, inner), F32),
                dma((pieces + 1,)),
                dma((3,)),
                dma((n_tp, pieces)),
                dma((n_tp,)),
                dma((2, chips, pieces)),
                dma((chips, pieces)),
                dma((2, chips)),
                dma((chips,)),
                dma((seqs, n_sp)),
                dma((seqs, n_sp)),
            ],
            compiler_params=pltpu.CompilerParams(
                collective_id=0, has_side_effects=True, vmem_limit_bytes=60 * 1024 * 1024
            ),
            name="retention",
        )(tokens, new_token.reshape(seqs, feat), query_weight, key_weight, value_weight, inverse, log_decay)

    return jax.shard_map(
        body,
        mesh=mesh,
        in_specs=(
            P(None, "sp", "tp"),
            P(None, None, "tp"),
            P(None, "tp"),
            P(None, "tp"),
            P(None, "tp"),
            P("tp"),
        ),
        out_specs=(P(None, "tp", "sp", None), P(None, "tp")),
        check_vma=False,
    )
```
